32 devices in a mesh: kv: 16 (over z, y, x), tp: 2 (over core).
Axes of the slice: x: 2, y: 2, z: 4, core: 2. Of those that a mesh axis runs over, the one named last changes fastest.
Arguments:
- queries: bfloat16 [4096, 1024], P('kv', 'tp'), may hold values from -4 to 4
- keys: bfloat16 [4096, 1024], P('kv', 'tp'), may hold values from -4 to 4
- values: bfloat16 [4096, 1024], P('kv', 'tp'), may hold values from -5 to 5
- log_sums: float32 [16, 4096], P('tp', 'kv'), may hold values from 5.5 to 7
- out_grad: bfloat16 [4096, 1024], P('kv', 'tp'), may hold values from -24 to 24
- chosen: int32 [32, 8], P('kv'), may hold values from -1 to 127, as said below
- normed: bfloat16 [4096, 2048], P('kv', 'tp'), may hold values from -0.23925781 to 0.23925781
Outputs:
- query_grad: bfloat16 [4096, 1024], P('kv', 'tp')
- key_grad: bfloat16 [4096, 1024], P('kv', 'tp')
- value_grad: bfloat16 [4096, 1024], P('kv', 'tp')
- weight_grad: float32 [2048, 1024], P('kv', 'tp')
The draws below stay inside these ranges and needn't reach their ends.
Inputs may be any that keep to these rules, and one draw needn't show every extreme that they name: `chosen`: each used entry names a key block that ends at or before its query block's start; the used entries of one list are distinct. Among the lists of the 2 query blocks of one index of kv, the key blocks of any other index of kv appear as at most one distinct block; for every index from 1 on, the first query block's list names a block of the index before, and the last index's first query block's list names a block of index 0. Blocks of the own index of kv before the query block may appear freely.
All inputs are finite; a program needn't handle non-finite values.
Results may differ from the reference program's by a relative error of at most 0.008.
Values may be sent and summed in bfloat16 or wider, within the bound.
A program may use at most 64 MiB of HBM per device.

```python
import jax
import jax.numpy as jnp
from jax import lax

D = 2048
HEADS = 16
HD = 64
QB = 128
KB = 32
SEL = 8
TOKENS = 4096
QBLK_DEV = 2
KBLK_DEV = 8
NQB = 32
KEY_BLOCK_TOTAL = 128


def draw_chosen(key, part):
    device_count = KEY_BLOCK_TOTAL // KBLK_DEV
    first_key, second_key, third_key, fourth_key = jax.random.split(key, 4)
    favoured = jax.random.randint(first_key, (device_count,), 0, KBLK_DEV, dtype=jnp.int32)
    spread_pick = jax.random.randint(second_key, (device_count, device_count), 0, KBLK_DEV, dtype=jnp.int32)
    coin_toss = jax.random.randint(third_key, (device_count, device_count), 0, 4, dtype=jnp.int32)
    pool_offset = jnp.where(coin_toss < 3, favoured[None, :], spread_pick)
    block_numbers = jnp.arange(KEY_BLOCK_TOTAL, dtype=jnp.int32)
    query_ids = jnp.arange(NQB, dtype=jnp.int32)
    holder = (query_ids // QBLK_DEV)[:, None]
    inner = (query_ids % QBLK_DEV)[:, None]
    owner_ids = (block_numbers // KBLK_DEV)[None, :]
    offset_ids = (block_numbers % KBLK_DEV)[None, :]
    pool_pick = pool_offset[holder, owner_ids]
    from_pool = (owner_ids < holder) & (offset_ids == pool_pick)
    from_own = (owner_ids == holder) & (offset_ids < inner * (QB // KB))
    eligible_blocks = from_pool | from_own
    rank_order = jax.random.randint(fourth_key, (NQB, KEY_BLOCK_TOTAL), 0, 4096, dtype=jnp.int32)
    preceding_single = (owner_ids == holder - 1) & (inner == 0)
    halfway_distance = (owner_ids == holder - device_count // 2) & (inner == min(1, QBLK_DEV - 1))
    farthest_pair = (owner_ids == 0) & (holder == device_count - 1) & (inner == 0)
    extra_reward = jnp.where(preceding_single | halfway_distance | farthest_pair, 8192, 0).astype(jnp.int32)
    graded_blocks = jnp.where(eligible_blocks, (rank_order + extra_reward) * KEY_BLOCK_TOTAL + block_numbers[None, :], -1).astype(jnp.int32)
    top_scores, top_ids = lax.top_k(graded_blocks, SEL)
    return jnp.where(top_scores >= 0, top_ids, -1).astype(jnp.int32)


def with_spikes(drawn, rng, source, target, shards_of, factor):
    owner, partner = [(jnp.arange(drawn.shape[axis_at]) // (drawn.shape[axis_at] // shards_of)).reshape([-1 if axis == axis_at else 1 for axis in range(drawn.ndim)]) for axis_at in (source, target)]
    chosen = jax.random.permutation(rng, shards_of)[partner]
    strong = (owner == chosen) | (owner == (partner + shards_of // 2) % shards_of)
    return jnp.where(strong, factor * drawn, drawn)


def block_scale(own_key, dims, shards, least, high):
    gain, own = 1.0, jax.random.fold_in(own_key, 6)
    for dim, blocks in shards:
        steps = jnp.exp(jax.random.uniform(jax.random.fold_in(own, dim), (blocks,), jnp.float32, least / len(shards), high / len(shards)))
        gain = gain * jnp.repeat(steps, dims[dim] // blocks).reshape([-1 if axis == dim else 1 for axis in range(len(dims))])
    return gain


def gaussian(own_key, shape, deviation, limit, cuts=(), kind=jnp.bfloat16):
    result = deviation * jax.random.normal(own_key, shape, jnp.float32)
    if cuts:
        result = result * block_scale(own_key, shape, cuts, -0.22, 0.18)
    return jnp.clip(result, -limit, limit).astype(kind)


def heavy_noise(stream_key, shape, scale, bound, cuts, heavy, held_as=jnp.bfloat16):
    values = scale * jax.random.normal(stream_key, shape, jnp.float32)
    if cuts:
        values = values * block_scale(stream_key, shape, cuts, -0.22, 0.18)
    return jnp.clip(with_spikes(values, jax.random.fold_in(stream_key, 3), *heavy), -bound, bound).astype(held_as)


def setup_inputs(seed: int = 0) -> dict:
    splits = jax.random.split(jax.random.key(seed), 8)
    queries = gaussian(splits[0], (TOKENS, HEADS * HD), 1.0, 4.0, ((0, 16), (1, 2)))
    keys = gaussian(splits[1], (TOKENS, HEADS * HD), 1.0, 4.0, ((0, 16), (1, 2)))
    values = gaussian(splits[2], (TOKENS, HEADS * HD), 1.0, 5.0, ((0, 16), (1, 2)))
    log_sums = jnp.clip(5.5 + 1.5 * jax.random.uniform(splits[3], (HEADS, TOKENS), jnp.float32) ** block_scale(splits[3], (HEADS, TOKENS), ((0, 2), (1, 16)), -0.2, 0.2), 5.5, 7.0)
    out_grad = gaussian(splits[4], (TOKENS, HEADS * HD), 4.0, 24.0, ((0, 16), (1, 2)))
    chosen = draw_chosen(jax.random.fold_in(splits[7], 71), 0)
    normed = heavy_noise(splits[6], (TOKENS, D), 0.03, 0.23925781, ((0, 16), (1, 2)), (0, 1, 16, 2.0))
    return {"queries": queries, "keys": keys, "values": values, "log_sums": log_sums, "out_grad": out_grad, "chosen": chosen, "normed": normed}


def rounded(array):
    return lax.optimization_barrier(array.astype(jnp.bfloat16)).astype(jnp.float32)


def block_grads(inputs, scaling):
    query_blk, grad_blk, sums_blk, keys_sel, vals_sel, keys_own, vals_own, eligible_blocks = inputs
    span_rows = query_blk.shape[0]
    scores = jnp.einsum("qhd,skhd->hqsk", query_blk, keys_sel) * scaling
    weights = jnp.where(eligible_blocks[None, None, :, None], jnp.exp(scores - sums_blk[:, :, None, None]), 0.0)
    causal = lax.broadcasted_iota(jnp.int32, (span_rows, span_rows), 0) >= lax.broadcasted_iota(jnp.int32, (span_rows, span_rows), 1)
    own_scores = jnp.einsum("qhd,khd->hqk", query_blk, keys_own) * scaling
    own_weights = jnp.where(causal[None], jnp.exp(own_scores - sums_blk[:, :, None]), 0.0)
    weights_low = rounded(weights)
    own_low = rounded(own_weights)
    attended = jnp.einsum("hqsk,skhd->qhd", weights_low, vals_sel) + jnp.einsum("hqk,khd->qhd", own_low, vals_own)
    deltas = jnp.sum(grad_blk * attended, axis=-1).T
    dots_sel = jnp.einsum("qhd,skhd->hqsk", grad_blk, vals_sel)
    own_dots = jnp.einsum("qhd,khd->hqk", grad_blk, vals_own)
    slopes = rounded(weights * (dots_sel - deltas[:, :, None, None]))
    own_slopes = rounded(own_weights * (own_dots - deltas[:, :, None]))
    query_part = scaling * (jnp.einsum("hqsk,skhd->qhd", slopes, keys_sel) + jnp.einsum("hqk,khd->qhd", own_slopes, keys_own))
    key_terms = scaling * jnp.einsum("hqsk,qhd->skhd", slopes, query_blk)
    value_terms = jnp.einsum("hqsk,qhd->skhd", weights_low, grad_blk)
    own_key_terms = scaling * jnp.einsum("hqk,qhd->khd", own_slopes, query_blk)
    own_value_terms = jnp.einsum("hqk,qhd->khd", own_low, grad_blk)
    return query_part.astype(jnp.bfloat16), key_terms, value_terms, own_key_terms, own_value_terms


def reference(queries, keys, values, log_sums, out_grad, chosen, normed):
    rows_all, columns = queries.shape
    head_count = log_sums.shape[0]
    head_size = columns // head_count
    query_blocks = rows_all // QB
    key_blocks = rows_all // KB
    selected = chosen.shape[1]
    scaling = head_size ** -0.5
    eligible_blocks = chosen >= 0
    picked = jnp.clip(chosen, 0, key_blocks - 1).astype(jnp.int32)
    query_full = queries.astype(jnp.float32).reshape(rows_all, head_count, head_size)
    key_full = keys.astype(jnp.float32).reshape(rows_all, head_count, head_size)
    value_full = values.astype(jnp.float32).reshape(rows_all, head_count, head_size)
    grad_full = out_grad.astype(jnp.float32).reshape(rows_all, head_count, head_size)
    offsets_kb = jnp.arange(KB, dtype=jnp.int32)

    def step(carry, index):
        key_acc, value_acc = carry
        first_row = (index * QB).astype(jnp.int32)
        query_blk = lax.dynamic_slice_in_dim(query_full, first_row, QB, 0)
        grad_blk = lax.dynamic_slice_in_dim(grad_full, first_row, QB, 0)
        sums_blk = lax.dynamic_slice_in_dim(log_sums, first_row, QB, 1)
        rows_sel = (picked[index][:, None] * KB + offsets_kb[None, :]).reshape(-1)
        keys_sel = key_full[rows_sel].reshape(selected, KB, head_count, head_size)
        vals_sel = value_full[rows_sel].reshape(selected, KB, head_count, head_size)
        keys_own = lax.dynamic_slice_in_dim(key_full, first_row, QB, 0)
        vals_own = lax.dynamic_slice_in_dim(value_full, first_row, QB, 0)
        query_part, key_terms, value_terms, own_key_terms, own_value_terms = block_grads(
            (query_blk, grad_blk, sums_blk, keys_sel, vals_sel, keys_own, vals_own, eligible_blocks[index]), scaling)
        key_acc = key_acc.at[rows_sel].add(key_terms.reshape(-1, head_count, head_size))
        value_acc = value_acc.at[rows_sel].add(value_terms.reshape(-1, head_count, head_size))
        key_acc = lax.dynamic_update_slice_in_dim(key_acc, lax.dynamic_slice_in_dim(key_acc, first_row, QB, 0) + own_key_terms, first_row, 0)
        value_acc = lax.dynamic_update_slice_in_dim(value_acc, lax.dynamic_slice_in_dim(value_acc, first_row, QB, 0) + own_value_terms, first_row, 0)
        return (key_acc, value_acc), query_part

    zeros_acc = jnp.zeros((rows_all, head_count, head_size), jnp.float32)
    (key_acc, value_acc), query_parts = lax.scan(step, (zeros_acc, zeros_acc), jnp.arange(query_blocks, dtype=jnp.int32))
    query_grad = query_parts.reshape(rows_all, columns)
    key_grad = key_acc.reshape(rows_all, columns).astype(jnp.bfloat16)
    value_grad = value_acc.reshape(rows_all, columns).astype(jnp.bfloat16)
    weight_grad = jnp.dot(normed.T, value_grad, preferred_element_type=jnp.float32)
    return query_grad, key_grad, value_grad, weight_grad
```

```python
from functools import partial

import jax
import jax.numpy as jnp
from jax import lax
from jax.experimental import pallas as pl
from jax.experimental.pallas import tpu as pltpu
from jax.sharding import PartitionSpec as P

QB = 128
KB = 32
LANES = 128
CHUNK = 256
NEG = -1e30
F32 = jnp.float32
BF16 = jnp.bfloat16


def dot(a, b, ca, cb):
    return lax.dot_general(a, b, (((ca,), (cb,)), ((), ())), preferred_element_type=F32)


def kernel(
    n, nt, hs,
    q_ref, k_ref, v_ref, lse_ref, g_ref, req_ref, used_ref, x_ref,
    qg_ref, kg_ref, vg_ref, wg_ref,
    reqbox, sel, outk, outv, kall, vall, rvo, rko, rvi, rki, wscr, ownv, ownk, bias, xall, wpart, win,
    req_s, req_r, k_s, k_r, v_s, v_r, vt_s, vt_r, kt_s, kt_r, w_s, w_r, x_s, x_r,
):
    me = lax.axis_index("kv")
    mt = lax.axis_index("tp")
    rows, cols = q_ref.shape
    nf = n * KB
    feats = x_ref.shape[1]
    wrows = wg_ref.shape[0]
    scale = hs ** (-0.5)
    hp = LANES // hs

    def rcopy(src, dst, ss, rs, dev):
        return pltpu.make_async_remote_copy(
            src_ref=src, dst_ref=dst, send_sem=ss, recv_sem=rs,
            device_id=dev, device_id_type=pl.DeviceIdType.MESH,
        )

    def slot(ref, i):
        return ref.at[pl.ds(pl.multiple_of(i * KB, KB), KB)]

    reqbox[...] = jnp.zeros_like(reqbox)
    kall[0:nf] = jnp.zeros((nf, cols), BF16)
    vall[0:nf] = jnp.zeros((nf, cols), BF16)
    rvi[...] = jnp.zeros_like(rvi)
    rki[...] = jnp.zeros_like(rki)

    barrier = pltpu.get_barrier_semaphore()

    @pl.loop(1, n)
    def _(d):
        pl.semaphore_signal(barrier, inc=1, device_id={"kv": lax.rem(me + d, n)},
                            device_id_type=pl.DeviceIdType.MESH)

    @pl.loop(1, nt)
    def _(d):
        pl.semaphore_signal(barrier, inc=1, device_id={"tp": lax.rem(mt + d, nt)},
                            device_id_type=pl.DeviceIdType.MESH)

    pl.semaphore_wait(barrier, n - 1 + nt - 1)

    def req_copy(src_i, dst_i):
        return rcopy(req_ref, reqbox.at[src_i], req_s.at[dst_i], req_r.at[src_i], {"kv": dst_i})

    def k_copy(src_i, dst_i):
        return rcopy(slot(outk, dst_i), slot(kall, src_i), k_s.at[dst_i], k_r.at[src_i], {"kv": dst_i})

    def v_copy(src_i, dst_i):
        return rcopy(slot(outv, dst_i), slot(vall, src_i), v_s.at[dst_i], v_r.at[src_i], {"kv": dst_i})

    def vt_copy(src_i, dst_i):
        return rcopy(slot(rvo, dst_i), slot(rvi, src_i), vt_s.at[dst_i], vt_r.at[src_i], {"kv": dst_i})

    def kt_copy(src_i, dst_i):
        return rcopy(slot(rko, dst_i), slot(rki, src_i), kt_s.at[dst_i], kt_r.at[src_i], {"kv": dst_i})

    def w_copy(src_i, dst_i):
        return rcopy(wpart.at[pl.ds(pl.multiple_of(dst_i * wrows, wrows), wrows)], win.at[src_i],
                     w_s.at[dst_i], w_r.at[src_i], {"kv": dst_i})

    def x_copy(src_t, dst_t):
        return rcopy(x_ref, xall.at[src_t], x_s.at[dst_t], x_r.at[src_t], {"tp": dst_t})

    @pl.loop(0, me)
    def _(j):
        req_copy(me, j).start()

    @pl.loop(1, nt)
    def _(d):
        x_copy(mt, lax.rem(mt + d, nt)).start()

    kall[nf:] = k_ref[...]
    vall[nf:] = v_ref[...]
    xall[mt] = x_ref[...]
    used = used_ref[...]
    nslots = used.shape[0]
    bias[...] = jnp.broadcast_to(used, (nslots, KB, rows)).reshape(nslots * KB, rows)
    kpos = lax.broadcasted_iota(jnp.int32, (rows, rows), 0)
    qpos = lax.broadcasted_iota(jnp.int32, (rows, rows), 1)
    causal = (kpos <= qpos) & (kpos // QB == qpos // QB)
    bias[nf:] = jnp.where(causal, 0.0, bias[nf:])

    @pl.loop(me + 1, n)
    def _(i):
        req_copy(i, me).wait_recv()

    box = reqbox[:, 0:1, :]
    lane = lax.broadcasted_iota(jnp.int32, box.shape, 2)
    off = jnp.sum(jnp.where(lane == me, box, 0), axis=2, keepdims=True)
    row3 = lax.broadcasted_iota(jnp.int32, (n, KB, rows), 1)
    col3 = lax.broadcasted_iota(jnp.int32, (n, KB, rows), 2)
    hit = jnp.where(col3 == (off - 1) * KB + row3, 1.0, 0.0)
    sel[...] = hit.reshape(nf, rows).astype(BF16)

    outk[...] = dot(sel[...], k_ref[...], 1, 0).astype(BF16)

    @pl.loop(me + 1, n)
    def _(i):
        k_copy(me, i).start()

    outv[...] = dot(sel[...], v_ref[...], 1, 0).astype(BF16)

    @pl.loop(me + 1, n)
    def _(i):
        v_copy(me, i).start()

    lane_ids = lax.broadcasted_iota(jnp.int32, (1, LANES), 1)
    masks = [
        jnp.where((lane_ids >= s * hs) & (lane_ids < (s + 1) * hs), 1.0, 0.0).astype(BF16)
        for s in range(hp)
    ]

    @pl.loop(0, me)
    def _(j):
        k_copy(j, me).wait_recv()

    for p in range(cols // LANES):
        at = slice(p * LANES, (p + 1) * LANES)
        qp = q_ref[:, at] * jnp.asarray(scale, BF16)
        gp = g_ref[:, at]
        kp = kall[:, at]
        terms = None
        for s in range(hp):
            h = p * hp + s
            scores = dot(kp, qp * masks[s], 1, 1)
            w = jnp.exp(scores + (bias[...] - lse_ref[h:h + 1, :]))
            wscr[h] = w
            term = dot(w.astype(BF16), gp * masks[s], 1, 0)
            terms = term if terms is None else terms + term
        rvo[:, at] = terms[:nf].astype(BF16)
        ownv[:, at] = terms[nf:]

    @pl.loop(0, me)
    def _(j):
        vt_copy(me, j).start()

    @pl.loop(0, me)
    def _(j):
        v_copy(j, me).wait_recv()

    sub = lax.broadcasted_iota(jnp.int32, (LANES, rows), 0)
    for p in range(cols // LANES):
        at = slice(p * LANES, (p + 1) * LANES)
        qp = q_ref[:, at] * jnp.asarray(scale, BF16)
        gp = g_ref[:, at]
        kp = kall[:, at]
        vp = vall[:, at]
        terms = None
        grads = None
        for s in range(hp):
            h = p * hp + s
            dots = dot(vp, gp * masks[s], 1, 1)
            w = wscr[h]
            deltas = jnp.sum(w.astype(BF16).astype(F32) * dots, axis=0, keepdims=True)
            slopes = (w * (dots - deltas)).astype(BF16)
            term = dot(slopes, qp * masks[s], 1, 0)
            terms = term if terms is None else terms + term
            part = dot(kp, slopes, 0, 0)
            grads = part if grads is None else jnp.where(sub >= s * hs, part, grads)
        rko[:, at] = terms[:nf].astype(BF16)
        ownk[:, at] = terms[nf:]
        qg_ref[:, at] = (grads * scale).T.astype(BF16)

    @pl.loop(0, me)
    def _(j):
        kt_copy(me, j).start()

    @pl.loop(me + 1, n)
    def _(i):
        vt_copy(i, me).wait_recv()

    vg = (ownv[...] + dot(sel[...], rvi[...], 0, 0)).astype(BF16)
    vg_ref[...] = vg

    @pl.loop(1, nt)
    def _(d):
        x_copy(lax.rem(mt + d, nt), mt).wait_recv()

    width = min(CHUNK, feats)
    for t in range(nt):
        for c in range(feats // width):
            piece = dot(xall[t, :, c * width:(c + 1) * width], vg, 0, 0)
            wpart[t * feats + c * width:t * feats + (c + 1) * width, :] = piece.astype(BF16)

    @pl.loop(1, n)
    def _(d):
        w_copy(me, lax.rem(me + d, n)).start()

    @pl.loop(me + 1, n)
    def _(i):
        kt_copy(i, me).wait_recv()

    kg_ref[...] = (ownk[...] + dot(sel[...], rki[...], 0, 0)).astype(BF16)

    wg_ref[...] = wpart[pl.ds(pl.multiple_of(me * wrows, wrows), wrows), :].astype(F32)

    @pl.loop(1, n)
    def _(d):
        i = lax.rem(me + n - d, n)
        w_copy(i, me).wait_recv()
        wg_ref[...] += win[i].astype(F32)

    @pl.loop(0, me)
    def _(j):
        req_copy(me, j).wait_send()
        vt_copy(me, j).wait_send()
        kt_copy(me, j).wait_send()

    @pl.loop(me + 1, n)
    def _(i):
        k_copy(me, i).wait_send()
        v_copy(me, i).wait_send()

    @pl.loop(1, n)
    def _(d):
        w_copy(me, lax.rem(me + d, n)).wait_send()

    @pl.loop(1, nt)
    def _(d):
        x_copy(mt, lax.rem(mt + d, nt)).wait_send()


def body(n, nt, queries, keys, values, log_sums, out_grad, chosen, normed):
    me = lax.axis_index("kv")
    rows, cols = queries.shape
    heads = log_sums.shape[0]
    hs = cols // heads
    key_blocks = rows // KB
    nf = n * KB
    feats = normed.shape[1]
    wrows = feats * nt // n
    owners = chosen // key_blocks
    offsets = chosen % key_blocks
    valid = chosen >= 0
    remote = valid & (owners != me)
    ids = jnp.where(remote, owners, jnp.where(valid, n + offsets, -1))
    lanes = jnp.arange(LANES, dtype=jnp.int32)
    wanted = jnp.max(
        jnp.where(remote[:, :, None] & (owners[:, :, None] == lanes), offsets[:, :, None] + 1, 0),
        axis=(0, 1),
    )
    req = jnp.broadcast_to(wanted[None, :], (8, LANES))
    slots = jnp.arange(n + key_blocks, dtype=jnp.int32)
    use = jnp.any(ids[:, :, None] == slots, axis=1).T
    used = jnp.repeat(jnp.where(use, 0.0, NEG).astype(F32), QB, axis=1)[:, None, :]
    vmem = pl.BlockSpec(memory_space=pltpu.VMEM)
    dma = pltpu.SemaphoreType.DMA
    return pl.pallas_call(
        partial(kernel, n, nt, hs),
        out_shape=(
            jax.ShapeDtypeStruct((rows, cols), BF16),
            jax.ShapeDtypeStruct((rows, cols), BF16),
            jax.ShapeDtypeStruct((rows, cols), BF16),
            jax.ShapeDtypeStruct((wrows, cols), F32),
        ),
        in_specs=[vmem] * 8,
        out_specs=(vmem,) * 4,
        scratch_shapes=[
            pltpu.VMEM((n, 8, LANES), jnp.int32),
            pltpu.VMEM((nf, rows), BF16),
            pltpu.VMEM((nf, cols), BF16),
            pltpu.VMEM((nf, cols), BF16),
            pltpu.VMEM((nf + rows, cols), BF16),
            pltpu.VMEM((nf + rows, cols), BF16),
            pltpu.VMEM((nf, cols), BF16),
            pltpu.VMEM((nf, cols), BF16),
            pltpu.VMEM((nf, cols), BF16),
            pltpu.VMEM((nf, cols), BF16),
            pltpu.VMEM((heads, nf + rows, rows), F32),
            pltpu.VMEM((rows, cols), F32),
            pltpu.VMEM((rows, cols), F32),
            pltpu.VMEM((nf + rows, rows), F32),
            pltpu.VMEM((nt, rows, feats), BF16),
            pltpu.VMEM((n * wrows, cols), BF16),
            pltpu.VMEM((n, wrows, cols), BF16),
        ] + [dma((n,))] * 12 + [dma((nt,))] * 2,
        compiler_params=pltpu.CompilerParams(
            collective_id=0, has_side_effects=True, vmem_limit_bytes=60 * 1024 * 1024
        ),
    )(queries, keys, values, log_sums, out_grad, req, used, normed)


def solution(mesh):
    in_specs = (
        P("kv", "tp"),
        P("kv", "tp"),
        P("kv", "tp"),
        P("tp", "kv"),
        P("kv", "tp"),
        P("kv", None),
        P("kv", "tp"),
    )
    out_specs = (P("kv", "tp"), P("kv", "tp"), P("kv", "tp"), P("kv", "tp"))
    fn = partial(body, mesh.shape["kv"], mesh.shape["tp"])
    return jax.shard_map(fn, mesh=mesh, in_specs=in_specs, out_specs=out_specs, check_vma=False)
```

```python
from functools import partial

import jax
import jax.numpy as jnp
from jax import lax
from jax.experimental import pallas as pl
from jax.experimental.pallas import tpu as pltpu
from jax.sharding import PartitionSpec as P

QB = 128
KB = 32
LANES = 128
CHUNK = 256
PLANE = 4
PARTS = 2
NEG = -1e30
F32 = jnp.float32
BF16 = jnp.bfloat16


def dot(a, b, ca, cb):
    return lax.dot_general(a, b, (((ca,), (cb,)), ((), ())), preferred_element_type=F32)


def kernel(
    n, nt, hs,
    q_ref, k_ref, v_ref, lse_ref, g_ref, req_ref, used_ref, x_ref,
    qg_ref, kg_ref, vg_ref, wg_ref,
    reqbox, sel, outk, outv, kall, vall, rvo, rko, rvi, rki, wscr, ownv, ownk, bias, xall, wp, r1, r2, r3,
    req_s, req_r, k_s, k_r, v_s, v_r, vt_s, vt_r, kt_s, kt_r, a_s, a_r, b_s, b_r, c_s, c_r, x_s, x_r,
):
    me = lax.axis_index("kv")
    mt = lax.axis_index("tp")
    rows, cols = q_ref.shape
    nf = n * KB
    feats = x_ref.shape[1]
    wrows = wg_ref.shape[0]
    scale = hs ** (-0.5)
    hp = LANES // hs

    def rcopy(src, dst, ss, rs, dev):
        return pltpu.make_async_remote_copy(
            src_ref=src, dst_ref=dst, send_sem=ss, recv_sem=rs,
            device_id=dev, device_id_type=pl.DeviceIdType.MESH,
        )

    def slot(ref, i):
        return ref.at[pl.ds(pl.multiple_of(i * KB, KB), KB)]

    reqbox[...] = jnp.zeros_like(reqbox)
    kall[0:nf] = jnp.zeros((nf, cols), BF16)
    vall[0:nf] = jnp.zeros((nf, cols), BF16)
    rvi[...] = jnp.zeros_like(rvi)
    rki[...] = jnp.zeros_like(rki)
    wscr[:, 0:nf, :] = jnp.zeros((wscr.shape[0], nf, rows), F32)

    barrier = pltpu.get_barrier_semaphore()

    @pl.loop(1, n)
    def _(d):
        pl.semaphore_signal(barrier, inc=1, device_id={"kv": lax.rem(me + d, n)},
                            device_id_type=pl.DeviceIdType.MESH)

    @pl.loop(1, nt)
    def _(d):
        pl.semaphore_signal(barrier, inc=1, device_id={"tp": lax.rem(mt + d, nt)},
                            device_id_type=pl.DeviceIdType.MESH)

    pl.semaphore_wait(barrier, n - 1 + nt - 1)

    def req_copy(src_i, dst_i):
        return rcopy(req_ref, reqbox.at[src_i], req_s.at[dst_i], req_r.at[src_i], {"kv": dst_i})

    def k_copy(src_i, dst_i):
        return rcopy(slot(outk, dst_i), slot(kall, src_i), k_s.at[dst_i], k_r.at[src_i], {"kv": dst_i})

    def v_copy(src_i, dst_i):
        return rcopy(slot(outv, dst_i), slot(vall, src_i), v_s.at[dst_i], v_r.at[src_i], {"kv": dst_i})

    def vt_copy(src_i, dst_i):
        return rcopy(slot(rvo, dst_i), slot(rvi, src_i), vt_s.at[dst_i], vt_r.at[src_i], {"kv": dst_i})

    def kt_copy(src_i, dst_i):
        return rcopy(slot(rko, dst_i), slot(rki, src_i), kt_s.at[dst_i], kt_r.at[src_i], {"kv": dst_i})

    xb = lax.rem(me, 2)
    yb = lax.rem(lax.div(me, 2), 2)
    zi = lax.div(me, PLANE)
    nz = n // PLANE
    parts = wp.shape[0]
    wrp = wrows // parts
    px = me + 1 - 2 * xb
    py = me + 2 - 4 * yb

    def order(p):
        return (xb, yb, px, py) if p % 2 == 0 else (yb, xb, py, px)

    def a_copy(p):
        f, _, peer, _ = order(p)
        return rcopy(wp.at[p, pl.ds((1 - f) * 2, 2)], r1.at[p], a_s.at[p], a_r.at[p], {"kv": peer})

    def b_copy(p):
        f, g, _, peer = order(p)
        return rcopy(wp.at[p, f * 2 + 1 - g], r2.at[p], b_s.at[p], b_r.at[p], {"kv": peer})

    def c_copy(p, src_z, dst_z):
        f, g, _, _ = order(p)
        return rcopy(wp.at[p, f * 2 + g, dst_z], r3.at[p, src_z], c_s.at[p, dst_z], c_r.at[p, src_z],
                     {"kv": me + (dst_z - zi) * PLANE})

    def x_copy(src_t, dst_t):
        return rcopy(x_ref, xall.at[src_t], x_s.at[dst_t], x_r.at[src_t], {"tp": dst_t})

    @pl.loop(0, me)
    def _(j):
        req_copy(me, j).start()

    @pl.loop(1, nt)
    def _(d):
        x_copy(mt, lax.rem(mt + d, nt)).start()

    kall[nf:] = k_ref[...]
    vall[nf:] = v_ref[...]
    xall[mt] = x_ref[...]
    used = used_ref[...]
    nslots = used.shape[0]
    bias[...] = jnp.broadcast_to(used, (nslots, KB, rows)).reshape(nslots * KB, rows)
    kpos = lax.broadcasted_iota(jnp.int32, (rows, rows), 0)
    qpos = lax.broadcasted_iota(jnp.int32, (rows, rows), 1)
    causal = (kpos <= qpos) & (kpos // QB == qpos // QB)
    bias[nf:] = jnp.where(causal, 0.0, bias[nf:])

    lane_ids = lax.broadcasted_iota(jnp.int32, (1, LANES), 1)
    masks = [
        jnp.where((lane_ids >= s * hs) & (lane_ids < (s + 1) * hs), 1.0, 0.0).astype(BF16)
        for s in range(hp)
    ]

    def scan_keys(start, size):
        here = pl.ds(start, size)
        outs = []
        for p in range(cols // LANES):
            at = slice(p * LANES, (p + 1) * LANES)
            qp = q_ref[:, at] * jnp.asarray(scale, BF16)
            gp = g_ref[:, at]
            kp = kall[here, at]
            terms = None
            for s in range(hp):
                h = p * hp + s
                scores = dot(kp, qp * masks[s], 1, 1)
                w = jnp.exp(scores + (bias[here, :] - lse_ref[h:h + 1, :]))
                wscr[h, here, :] = w
                term = dot(w.astype(BF16), gp * masks[s], 1, 0)
                terms = term if terms is None else terms + term
            outs.append((at, terms))
        return outs

    for at, terms in scan_keys(nf, rows):
        ownv[:, at] = terms

    @pl.loop(me + 1, n)
    def _(i):
        req_copy(i, me).wait_recv()

    box = reqbox[:, 0:1, :]
    lane = lax.broadcasted_iota(jnp.int32, box.shape, 2)
    off = jnp.sum(jnp.where(lane == me, box, 0), axis=2, keepdims=True)
    row3 = lax.broadcasted_iota(jnp.int32, (n, KB, rows), 1)
    col3 = lax.broadcasted_iota(jnp.int32, (n, KB, rows), 2)
    hit = jnp.where(col3 == (off - 1) * KB + row3, 1.0, 0.0)
    sel[...] = hit.reshape(nf, rows).astype(BF16)

    outk[...] = dot(sel[...], k_ref[...], 1, 0).astype(BF16)

    @pl.loop(me + 1, n)
    def _(i):
        k_copy(me, i).start()

    outv[...] = dot(sel[...], v_ref[...], 1, 0).astype(BF16)

    @pl.loop(me + 1, n)
    def _(i):
        v_copy(me, i).start()

    def group(first, end):
        @pl.loop(first, end)
        def _(j):
            k_copy(j, me).wait_recv()

        start = pl.multiple_of(first * KB, PLANE * KB)
        for at, terms in scan_keys(start, PLANE * KB):
            rvo[pl.ds(start, PLANE * KB), at] = terms.astype(BF16)

        @pl.loop(first, end)
        def _(j):
            vt_copy(me, j).start()

    group(zi * PLANE, me)

    @pl.loop(0, zi)
    def _(t):
        first = (zi - 1 - t) * PLANE
        group(first, first + PLANE)

    @pl.loop(me + 1, n)
    def _(i):
        vt_copy(i, me).wait_recv()

    vg = (ownv[...] + dot(sel[...], rvi[...], 0, 0)).astype(BF16)
    vg_ref[...] = vg

    @pl.loop(1, nt)
    def _(d):
        x_copy(lax.rem(mt + d, nt), mt).wait_recv()

    width = min(CHUNK, feats)
    for t in range(nt):
        for c in range(feats // width):
            piece = dot(xall[t, :, c * width:(c + 1) * width], vg, 0, 0).astype(BF16)
            for r in range(width // wrows):
                i = (t * feats + c * width) // wrows + r
                bx, by, bz = i % 2, (i // 2) % 2, i // PLANE
                for p in range(parts):
                    to = bx * 2 + by if p % 2 == 0 else by * 2 + bx
                    wp[p, to, bz] = piece[r * wrows + p * wrp:r * wrows + (p + 1) * wrp, :]

    for p in range(parts):
        a_copy(p).start()

    @pl.loop(0, me)
    def _(j):
        v_copy(j, me).wait_recv()

    sub = lax.broadcasted_iota(jnp.int32, (LANES, rows), 0)
    for p in range(cols // LANES):
        at = slice(p * LANES, (p + 1) * LANES)
        qp = q_ref[:, at] * jnp.asarray(scale, BF16)
        gp = g_ref[:, at]
        kp = kall[:, at]
        vp = vall[:, at]
        terms = None
        grads = None
        for s in range(hp):
            h = p * hp + s
            dots = dot(vp, gp * masks[s], 1, 1)
            w = wscr[h]
            deltas = jnp.sum(w.astype(BF16).astype(F32) * dots, axis=0, keepdims=True)
            slopes = (w * (dots - deltas)).astype(BF16)
            term = dot(slopes, qp * masks[s], 1, 0)
            terms = term if terms is None else terms + term
            part = dot(kp, slopes, 0, 0)
            grads = part if grads is None else jnp.where(sub >= s * hs, part, grads)
        rko[:, at] = terms[:nf].astype(BF16)
        ownk[:, at] = terms[nf:]
        qg_ref[:, at] = (grads * scale).T.astype(BF16)

    @pl.loop(0, me)
    def _(j):
        kt_copy(me, j).start()

    for p in range(parts):
        f, g, _, _ = order(p)
        a_copy(p).wait()
        half = wp[p, pl.ds(f * 2, 2)].astype(F32) + r1[p].astype(F32)
        wp[p, pl.ds(f * 2, 2)] = half.astype(BF16)
        b_copy(p).start()

    for p in range(parts):
        f, g, _, _ = order(p)
        b_copy(p).wait()
        mine = wp[p, f * 2 + g].astype(F32) + r2[p].astype(F32)
        wp[p, f * 2 + g] = mine.astype(BF16)

        @pl.loop(1, nz)
        def _(e):
            c_copy(p, zi, lax.rem(zi + e, nz)).start()

    @pl.loop(me + 1, n)
    def _(i):
        kt_copy(i, me).wait_recv()

    kg_ref[...] = (ownk[...] + dot(sel[...], rki[...], 0, 0)).astype(BF16)

    for p in range(parts):
        f, g, _, _ = order(p)
        at = slice(p * wrp, (p + 1) * wrp)
        wg_ref[at, :] = wp[p, f * 2 + g, zi].astype(F32)

        @pl.loop(1, nz)
        def _(e):
            src_z = lax.rem(zi + nz - e, nz)
            c_copy(p, src_z, zi).wait_recv()
            wg_ref[at, :] += r3[p, src_z].astype(F32)

    @pl.loop(0, me)
    def _(j):
        req_copy(me, j).wait_send()
        vt_copy(me, j).wait_send()
        kt_copy(me, j).wait_send()

    @pl.loop(me + 1, n)
    def _(i):
        k_copy(me, i).wait_send()
        v_copy(me, i).wait_send()

    for p in range(parts):
        @pl.loop(1, nz)
        def _(e):
            c_copy(p, zi, lax.rem(zi + e, nz)).wait_send()

    @pl.loop(1, nt)
    def _(d):
        x_copy(mt, lax.rem(mt + d, nt)).wait_send()


def body(n, nt, queries, keys, values, log_sums, out_grad, chosen, normed):
    me = lax.axis_index("kv")
    rows, cols = queries.shape
    heads = log_sums.shape[0]
    hs = cols // heads
    key_blocks = rows // KB
    nf = n * KB
    feats = normed.shape[1]
    wrows = feats * nt // n
    owners = chosen // key_blocks
    offsets = chosen % key_blocks
    valid = chosen >= 0
    remote = valid & (owners != me)
    ids = jnp.where(remote, owners, jnp.where(valid, n + offsets, -1))
    lanes = jnp.arange(LANES, dtype=jnp.int32)
    wanted = jnp.max(
        jnp.where(remote[:, :, None] & (owners[:, :, None] == lanes), offsets[:, :, None] + 1, 0),
        axis=(0, 1),
    )
    req = jnp.broadcast_to(wanted[None, :], (8, LANES))
    slots = jnp.arange(n + key_blocks, dtype=jnp.int32)
    use = jnp.any(ids[:, :, None] == slots, axis=1).T
    used = jnp.repeat(jnp.where(use, 0.0, NEG).astype(F32), QB, axis=1)[:, None, :]
    nz = n // PLANE
    wrp = wrows // PARTS
    vmem = pl.BlockSpec(memory_space=pltpu.VMEM)
    dma = pltpu.SemaphoreType.DMA
    return pl.pallas_call(
        partial(kernel, n, nt, hs),
        out_shape=(
            jax.ShapeDtypeStruct((rows, cols), BF16),
            jax.ShapeDtypeStruct((rows, cols), BF16),
            jax.ShapeDtypeStruct((rows, cols), BF16),
            jax.ShapeDtypeStruct((wrows, cols), F32),
        ),
        in_specs=[vmem] * 8,
        out_specs=(vmem,) * 4,
        scratch_shapes=[
            pltpu.VMEM((n, 8, LANES), jnp.int32),
            pltpu.VMEM((nf, rows), BF16),
            pltpu.VMEM((nf, cols), BF16),
            pltpu.VMEM((nf, cols), BF16),
            pltpu.VMEM((nf + rows, cols), BF16),
            pltpu.VMEM((nf + rows, cols), BF16),
            pltpu.VMEM((nf, cols), BF16),
            pltpu.VMEM((nf, cols), BF16),
            pltpu.VMEM((nf, cols), BF16),
            pltpu.VMEM((nf, cols), BF16),
            pltpu.VMEM((heads, nf + rows, rows), F32),
            pltpu.VMEM((rows, cols), F32),
            pltpu.VMEM((rows, cols), F32),
            pltpu.VMEM((nf + rows, rows), F32),
            pltpu.VMEM((nt, rows, feats), BF16),
            pltpu.VMEM((PARTS, PLANE, nz, wrp, cols), BF16),
            pltpu.VMEM((PARTS, 2, nz, wrp, cols), BF16),
            pltpu.VMEM((PARTS, nz, wrp, cols), BF16),
            pltpu.VMEM((PARTS, nz, wrp, cols), BF16),
        ] + [dma((n,))] * 10 + [dma((PARTS,))] * 4 + [dma((PARTS, nz))] * 2 + [dma((nt,))] * 2,
        compiler_params=pltpu.CompilerParams(
            collective_id=0, has_side_effects=True, vmem_limit_bytes=60 * 1024 * 1024
        ),
    )(queries, keys, values, log_sums, out_grad, req, used, normed)


def solution(mesh):
    in_specs = (
        P("kv", "tp"),
        P("kv", "tp"),
        P("kv", "tp"),
        P("tp", "kv"),
        P("kv", "tp"),
        P("kv", None),
        P("kv", "tp"),
    )
    out_specs = (P("kv", "tp"), P("kv", "tp"), P("kv", "tp"), P("kv", "tp"))
    fn = partial(body, mesh.shape["kv"], mesh.shape["tp"])
    return jax.shard_map(fn, mesh=mesh, in_specs=in_specs, out_specs=out_specs, check_vma=False)
```

```python
from functools import partial

import jax
import jax.numpy as jnp
from jax import lax
from jax.experimental import pallas as pl
from jax.experimental.pallas import tpu as pltpu
from jax.sharding import PartitionSpec as P

QB = 128
KB = 32
LANES = 128
CHUNK = 256
PLANE = 4
NEG = -1e30
F32 = jnp.float32
BF16 = jnp.bfloat16


def dot(a, b, ca, cb):
    return lax.dot_general(a, b, (((ca,), (cb,)), ((), ())), preferred_element_type=F32)


def kernel(
    n, nt, hs,
    q_ref, k_ref, v_ref, lse_ref, g_ref, req_ref, used_ref, x_ref,
    qg_ref, kg_ref, vg_ref, wg_ref,
    reqbox, sel, outk, outv, kall, vall, rvo, rko, rvi, rki, wscr, ownv, ownk, bias, xall, wp, r1, r2, r3,
    req_s, req_r, k_s, k_r, v_s, v_r, vt_s, vt_r, kt_s, kt_r, a_s, a_r, b_s, b_r, c_s, c_r, x_s, x_r,
):
    me = lax.axis_index("kv")
    mt = lax.axis_index("tp")
    rows, cols = q_ref.shape
    nf = n * KB
    feats = x_ref.shape[1]
    wrows = wg_ref.shape[0]
    scale = hs ** (-0.5)
    hp = LANES // hs

    def rcopy(src, dst, ss, rs, dev):
        return pltpu.make_async_remote_copy(
            src_ref=src, dst_ref=dst, send_sem=ss, recv_sem=rs,
            device_id=dev, device_id_type=pl.DeviceIdType.MESH,
        )

    def slot(ref, i):
        return ref.at[pl.ds(pl.multiple_of(i * KB, KB), KB)]

    reqbox[...] = jnp.zeros_like(reqbox)
    kall[0:nf] = jnp.zeros((nf, cols), BF16)
    vall[0:nf] = jnp.zeros((nf, cols), BF16)
    rvi[...] = jnp.zeros_like(rvi)
    rki[...] = jnp.zeros_like(rki)
    wscr[:, 0:nf, :] = jnp.zeros((wscr.shape[0], nf, rows), F32)

    barrier = pltpu.get_barrier_semaphore()

    @pl.loop(1, n)
    def _(d):
        pl.semaphore_signal(barrier, inc=1, device_id={"kv": lax.rem(me + d, n)},
                            device_id_type=pl.DeviceIdType.MESH)

    @pl.loop(1, nt)
    def _(d):
        pl.semaphore_signal(barrier, inc=1, device_id={"tp": lax.rem(mt + d, nt)},
                            device_id_type=pl.DeviceIdType.MESH)

    pl.semaphore_wait(barrier, n - 1 + nt - 1)

    def req_copy(src_i, dst_i):
        return rcopy(req_ref, reqbox.at[src_i], req_s.at[dst_i], req_r.at[src_i], {"kv": dst_i})

    def k_copy(src_i, dst_i):
        return rcopy(slot(outk, dst_i), slot(kall, src_i), k_s.at[dst_i], k_r.at[src_i], {"kv": dst_i})

    def v_copy(src_i, dst_i):
        return rcopy(slot(outv, dst_i), slot(vall, src_i), v_s.at[dst_i], v_r.at[src_i], {"kv": dst_i})

    def vt_copy(src_i, dst_i):
        return rcopy(slot(rvo, dst_i), slot(rvi, src_i), vt_s.at[dst_i], vt_r.at[src_i], {"kv": dst_i})

    def kt_copy(src_i, dst_i):
        return rcopy(slot(rko, dst_i), slot(rki, src_i), kt_s.at[dst_i], kt_r.at[src_i], {"kv": dst_i})

    xb = lax.rem(me, 2)
    yb = lax.rem(lax.div(me, 2), 2)
    zi = lax.div(me, PLANE)
    nz = n // PLANE
    parts = wp.shape[0]
    wrp = wrows // parts
    px = me + 1 - 2 * xb
    py = me + 2 - 4 * yb

    def order(p):
        return (xb, yb, px, py) if p % 2 == 0 else (yb, xb, py, px)

    def a_copy(p):
        f, _, peer, _ = order(p)
        return rcopy(wp.at[p, pl.ds((1 - f) * 2, 2)], r1.at[p], a_s.at[p], a_r.at[p], {"kv": peer})

    def b_copy(p):
        f, g, _, peer = order(p)
        return rcopy(wp.at[p, f * 2 + 1 - g], r2.at[p], b_s.at[p], b_r.at[p], {"kv": peer})

    def c_copy(p, src_z, dst_z):
        f, g, _, _ = order(p)
        return rcopy(wp.at[p, f * 2 + g, dst_z], r3.at[p, src_z], c_s.at[p, dst_z], c_r.at[p, src_z],
                     {"kv": me + (dst_z - zi) * PLANE})

    def x_copy(src_t, dst_t):
        return rcopy(x_ref, xall.at[src_t], x_s.at[dst_t], x_r.at[src_t], {"tp": dst_t})

    @pl.loop(0, me)
    def _(j):
        req_copy(me, j).start()

    @pl.loop(1, nt)
    def _(d):
        x_copy(mt, lax.rem(mt + d, nt)).start()

    kall[nf:] = k_ref[...]
    vall[nf:] = v_ref[...]
    xall[mt] = x_ref[...]
    used = used_ref[...]
    nslots = used.shape[0]
    bias[...] = jnp.broadcast_to(used, (nslots, KB, rows)).reshape(nslots * KB, rows)
    kpos = lax.broadcasted_iota(jnp.int32, (rows, rows), 0)
    qpos = lax.broadcasted_iota(jnp.int32, (rows, rows), 1)
    causal = (kpos <= qpos) & (kpos // QB == qpos // QB)
    bias[nf:] = jnp.where(causal, 0.0, bias[nf:])

    lane_ids = lax.broadcasted_iota(jnp.int32, (1, LANES), 1)
    masks = [
        jnp.where((lane_ids >= s * hs) & (lane_ids < (s + 1) * hs), 1.0, 0.0).astype(BF16)
        for s in range(hp)
    ]

    def scan_keys(start, size):
        here = pl.ds(start, size)
        outs = []
        for p in range(cols // LANES):
            at = slice(p * LANES, (p + 1) * LANES)
            qp = q_ref[:, at] * jnp.asarray(scale, BF16)
            gp = g_ref[:, at]
            kp = kall[here, at]
            terms = None
            for s in range(hp):
                h = p * hp + s
                scores = dot(kp, qp * masks[s], 1, 1)
                w = jnp.exp(scores + (bias[here, :] - lse_ref[h:h + 1, :]))
                wscr[h, here, :] = w
                term = dot(w.astype(BF16), gp * masks[s], 1, 0)
                terms = term if terms is None else terms + term
            outs.append((at, terms))
        return outs

    for at, terms in scan_keys(nf, rows):
        ownv[:, at] = terms

    @pl.loop(me + 1, n)
    def _(i):
        req_copy(i, me).wait_recv()

    box = reqbox[:, 0:1, :]
    lane = lax.broadcasted_iota(jnp.int32, box.shape, 2)
    off = jnp.sum(jnp.where(lane == me, box, 0), axis=2, keepdims=True)
    row3 = lax.broadcasted_iota(jnp.int32, (n, KB, rows), 1)
    col3 = lax.broadcasted_iota(jnp.int32, (n, KB, rows), 2)
    hit = jnp.where(col3 == (off - 1) * KB + row3, 1.0, 0.0)
    sel[...] = hit.reshape(nf, rows).astype(BF16)

    outk[...] = dot(sel[...], k_ref[...], 1, 0).astype(BF16)

    @pl.loop(me + 1, n)
    def _(i):
        k_copy(me, i).start()

    outv[...] = dot(sel[...], v_ref[...], 1, 0).astype(BF16)

    @pl.loop(me + 1, n)
    def _(i):
        v_copy(me, i).start()

    def group(first, end):
        @pl.loop(first, end)
        def _(j):
            k_copy(j, me).wait_recv()

        start = pl.multiple_of(first * KB, PLANE * KB)
        for at, terms in scan_keys(start, PLANE * KB):
            rvo[pl.ds(start, PLANE * KB), at] = terms.astype(BF16)

        @pl.loop(first, end)
        def _(j):
            vt_copy(me, j).start()

    group(zi * PLANE, me)

    @pl.loop(0, zi)
    def _(t):
        first = (zi - 1 - t) * PLANE
        group(first, first + PLANE)

    @pl.loop(me + 1, n)
    def _(i):
        vt_copy(i, me).wait_recv()

    vg = (ownv[...] + dot(sel[...], rvi[...], 0, 0)).astype(BF16)
    vg_ref[...] = vg

    @pl.loop(1, nt)
    def _(d):
        x_copy(lax.rem(mt + d, nt), mt).wait_recv()

    width = min(CHUNK, feats)
    for t in range(nt):
        for c in range(feats // width):
            piece = dot(xall[t, :, c * width:(c + 1) * width], vg, 0, 0).astype(BF16)
            for r in range(width // wrows):
                i = (t * feats + c * width) // wrows + r
                bx, by, bz = i % 2, (i // 2) % 2, i // PLANE
                for p in range(parts):
                    to = bx * 2 + by if p % 2 == 0 else by * 2 + bx
                    wp[p, to, bz] = piece[r * wrows + p * wrp:r * wrows + (p + 1) * wrp, :]

    for p in range(parts):
        a_copy(p).start()

    @pl.loop(0, me)
    def _(j):
        v_copy(j, me).wait_recv()

    sub = lax.broadcasted_iota(jnp.int32, (LANES, rows), 0)
    for p in range(cols // LANES):
        at = slice(p * LANES, (p + 1) * LANES)
        qp = q_ref[:, at] * jnp.asarray(scale, BF16)
        gp = g_ref[:, at]
        kp = kall[:, at]
        vp = vall[:, at]
        terms = None
        grads = None
        for s in range(hp):
            h = p * hp + s
            dots = dot(vp, gp * masks[s], 1, 1)
            w = wscr[h]
            deltas = jnp.sum(w.astype(BF16).astype(F32) * dots, axis=0, keepdims=True)
            slopes = (w * (dots - deltas)).astype(BF16)
            term = dot(slopes, qp * masks[s], 1, 0)
            terms = term if terms is None else terms + term
            part = dot(kp, slopes, 0, 0)
            grads = part if grads is None else jnp.where(sub >= s * hs, part, grads)
        rko[:, at] = terms[:nf].astype(BF16)
        ownk[:, at] = terms[nf:]
        qg_ref[:, at] = (grads * scale).T.astype(BF16)

    @pl.loop(0, me)
    def _(j):
        kt_copy(me, j).start()

    for p in range(parts):
        f, g, _, _ = order(p)
        a_copy(p).wait()
        half = wp[p, pl.ds(f * 2, 2)].astype(F32) + r1[p].astype(F32)
        wp[p, pl.ds(f * 2, 2)] = half.astype(BF16)
        b_copy(p).start()

    for p in range(parts):
        f, g, _, _ = order(p)
        b_copy(p).wait()
        mine = wp[p, f * 2 + g].astype(F32) + r2[p].astype(F32)
        wp[p, f * 2 + g] = mine.astype(BF16)

        @pl.loop(1, nz)
        def _(e):
            c_copy(p, zi, lax.rem(zi + e, nz)).start()

    @pl.loop(me + 1, n)
    def _(i):
        kt_copy(i, me).wait_recv()

    kg_ref[...] = (ownk[...] + dot(sel[...], rki[...], 0, 0)).astype(BF16)

    for p in range(parts):
        f, g, _, _ = order(p)
        at = slice(p * wrp, (p + 1) * wrp)
        wg_ref[at, :] = wp[p, f * 2 + g, zi].astype(F32)

        @pl.loop(1, nz)
        def _(e):
            src_z = lax.rem(zi + nz - e, nz)
            c_copy(p, src_z, zi).wait_recv()
            wg_ref[at, :] += r3[p, src_z].astype(F32)

    @pl.loop(0, me)
    def _(j):
        req_copy(me, j).wait_send()
        vt_copy(me, j).wait_send()
        kt_copy(me, j).wait_send()

    @pl.loop(me + 1, n)
    def _(i):
        k_copy(me, i).wait_send()
        v_copy(me, i).wait_send()

    for p in range(parts):
        @pl.loop(1, nz)
        def _(e):
            c_copy(p, zi, lax.rem(zi + e, nz)).wait_send()

    @pl.loop(1, nt)
    def _(d):
        x_copy(mt, lax.rem(mt + d, nt)).wait_send()


def settle(*refs):
    for src, dst in zip(refs[:4], refs[4:]):
        dst[...] = src[...]


def body(n, nt, queries, keys, values, log_sums, out_grad, chosen, normed):
    me = lax.axis_index("kv")
    rows, cols = queries.shape
    heads = log_sums.shape[0]
    hs = cols // heads
    key_blocks = rows // KB
    nf = n * KB
    feats = normed.shape[1]
    wrows = feats * nt // n
    owners = chosen // key_blocks
    offsets = chosen % key_blocks
    valid = chosen >= 0
    remote = valid & (owners != me)
    ids = jnp.where(remote, owners, jnp.where(valid, n + offsets, -1))
    lanes = jnp.arange(LANES, dtype=jnp.int32)
    wanted = jnp.max(
        jnp.where(remote[:, :, None] & (owners[:, :, None] == lanes), offsets[:, :, None] + 1, 0),
        axis=(0, 1),
    )
    req = jnp.broadcast_to(wanted[None, :], (8, LANES))
    slots = jnp.arange(n + key_blocks, dtype=jnp.int32)
    use = jnp.any(ids[:, :, None] == slots, axis=1).T
    used = jnp.repeat(jnp.where(use, 0.0, NEG).astype(F32), QB, axis=1)[:, None, :]
    nz = n // PLANE
    parts = 4 if wrows % 64 == 0 else 2
    wrp = wrows // parts
    vmem = pl.BlockSpec(memory_space=pltpu.VMEM)
    dma = pltpu.SemaphoreType.DMA
    outs = pl.pallas_call(
        partial(kernel, n, nt, hs),
        out_shape=(
            jax.ShapeDtypeStruct((rows, cols), BF16),
            jax.ShapeDtypeStruct((rows, cols), BF16),
            jax.ShapeDtypeStruct((rows, cols), BF16),
            jax.ShapeDtypeStruct((wrows, cols), F32),
        ),
        in_specs=[vmem] * 8,
        out_specs=(vmem,) * 4,
        scratch_shapes=[
            pltpu.VMEM((n, 8, LANES), jnp.int32),
            pltpu.VMEM((nf, rows), BF16),
            pltpu.VMEM((nf, cols), BF16),
            pltpu.VMEM((nf, cols), BF16),
            pltpu.VMEM((nf + rows, cols), BF16),
            pltpu.VMEM((nf + rows, cols), BF16),
            pltpu.VMEM((nf, cols), BF16),
            pltpu.VMEM((nf, cols), BF16),
            pltpu.VMEM((nf, cols), BF16),
            pltpu.VMEM((nf, cols), BF16),
            pltpu.VMEM((heads, nf + rows, rows), F32),
            pltpu.VMEM((rows, cols), F32),
            pltpu.VMEM((rows, cols), F32),
            pltpu.VMEM((nf + rows, rows), F32),
            pltpu.VMEM((nt, rows, feats), BF16),
            pltpu.VMEM((parts, PLANE, nz, wrp, cols), BF16),
            pltpu.VMEM((parts, 2, nz, wrp, cols), BF16),
            pltpu.VMEM((parts, nz, wrp, cols), BF16),
            pltpu.VMEM((parts, nz, wrp, cols), BF16),
        ] + [dma((n,))] * 10 + [dma((parts,))] * 4 + [dma((parts, nz))] * 2 + [dma((nt,))] * 2,
        compiler_params=pltpu.CompilerParams(
            collective_id=0, has_side_effects=True, vmem_limit_bytes=60 * 1024 * 1024
        ),
    )(queries, keys, values, log_sums, out_grad, req, used, normed)
    return pl.pallas_call(
        settle,
        out_shape=tuple(jax.ShapeDtypeStruct(o.shape, o.dtype) for o in outs),
        in_specs=[vmem] * 4,
        out_specs=(vmem,) * 4,
    )(*outs)


def solution(mesh):
    in_specs = (
        P("kv", "tp"),
        P("kv", "tp"),
        P("kv", "tp"),
        P("tp", "kv"),
        P("kv", "tp"),
        P("kv", None),
        P("kv", "tp"),
    )
    out_specs = (P("kv", "tp"), P("kv", "tp"), P("kv", "tp"), P("kv", "tp"))
    fn = partial(body, mesh.shape["kv"], mesh.shape["tp"])
    return jax.shard_map(fn, mesh=mesh, in_specs=in_specs, out_specs=out_specs, check_vma=False)
```
